32 devices in a mesh: grp: 2 (over y), sp: 4 (over z), fs: 2 (over x), tp: 2 (over core).
Axes of the slice: x: 2, y: 2, z: 4, core: 2. Of those that a mesh axis runs over, the one named last changes fastest.
Arguments:
- tokens: bfloat16 [2, 6144, 2048], P('fs', ('grp', 'sp'), 'tp'), parts along dimension 1, may hold values from -12 to 12
- norm_gain: float32 [2048], replicated, may hold values from 0.1 to 1.9
- query_weight: bfloat16 [2048, 16, 64], P(None, 'tp'), may hold values from -3 to 3
- key_weight: bfloat16 [2048, 4, 64], P(None, 'tp'), may hold values from -3 to 3
- value_weight: bfloat16 [2048, 4, 64], P(None, 'tp'), may hold values from -0.125 to 0.125
- sink_logit: float32 [16], P('tp'), may hold values from 1 to 6
- pool_weight: bfloat16 [2048, 4, 256], P(None, None, 'tp'), may hold values from -0.125 to 0.125
- attn_out_weight: bfloat16 [16, 64, 2048], P('tp'), may hold values from -0.5 to 0.5
- pool_out_weight: bfloat16 [4, 256, 2048], P(None, 'tp'), may hold values from -0.1875 to 0.1875
Outputs:
- mixed: bfloat16 [2, 6144, 2048], P('fs', ('grp', 'sp', 'tp')), parts along dimension 1
The draws below stay inside these ranges and needn't reach their ends.
There are 2 independent parts, one for each index of `grp`. The reference program is written for one: setup_inputs(seed, part) draws one part's arguments, and reference() takes and returns one part's arrays. A program takes and returns all parts, laid end to end along the dimension named above; an argument that names none is the same for every part. Nothing has to cross between parts.
All inputs are finite; a program needn't handle non-finite values.
Results may differ from the reference program's by a relative error of at most 0.0095.
The reference program's roundings to bfloat16 on the way (of `normed`, `weight`, `attended` and `pooled`) count: a program that leaves them out, or rounds other values in their place, can miss the bound.
Values may be sent and summed in bfloat16 or wider, within the bound.
No kernel may reach another device: no remote copies, remote signals or barrier semaphores. Data moves between devices by JAX's collectives and lax.ppermute only.
A program may use at most 128 MiB of HBM per device.

```python
import jax
import jax.numpy as jnp
from jax import lax

D = 2048
HEADS = 16
KV_HEADS = 4
HEAD_DIM = 64
POOL_CH = 256
WINDOW = 128
TOK_DEV = 768
SEQS = 2
LEN = 3072


def draw_tokens(key, part):
    first, second, third = jax.random.split(jax.random.fold_in(key, 11), 3)
    blocks = LEN // TOK_DEV
    base = jax.random.normal(first, (SEQS, blocks, TOK_DEV, D), jnp.float32)
    offset = jax.random.normal(second, (SEQS, 1, 1, D), jnp.float32)
    factor = jax.random.uniform(third, (SEQS, blocks, 1, 1), jnp.float32, -1.5, 1.5)
    values = jnp.clip(base + factor * offset, -12.0, 12.0)
    return values.reshape(SEQS, LEN, D).astype(jnp.bfloat16)


def projection(key, heads):
    values = jax.random.normal(key, (D, heads, HEAD_DIM), jnp.float32) * D ** (-0.5)
    return jnp.clip(values, -3.0, 3.0).astype(jnp.bfloat16)


def draw_query_weight(key, part):
    return projection(jax.random.fold_in(key, 21), HEADS)


def draw_key_weight(key, part):
    return projection(jax.random.fold_in(key, 31), KV_HEADS)


def block_levels(stream_key, extent, shards, low, top_value):
    def one(dim, blocks):
        heights = jax.random.uniform(jax.random.fold_in(jax.random.fold_in(stream_key, 6), dim), (blocks,), jnp.float32, low / len(shards), top_value / len(shards))
        return jnp.repeat(jnp.exp(heights), extent[dim] // blocks).reshape((-1,) + (1,) * (len(extent) - dim - 1))

    level = one(*shards[0])
    for cut in shards[1:]:
        level = level * one(*cut)
    return level


def noise(own_key, extent, deviation, limit, cuts=(), kind=jnp.bfloat16):
    loudness = block_levels(own_key, extent, cuts, -0.22, 0.18) if cuts else 1.0
    values = jax.random.normal(own_key, extent, jnp.float32) * deviation * loudness
    return jnp.minimum(jnp.maximum(values, -limit), limit).astype(kind)


def setup_inputs(seed: int = 0, part: int = 0) -> dict:
    streams_of = jax.random.split(jax.random.key(seed), 10)
    part_splits = jax.random.split(jax.random.fold_in(streams_of[9], part), 10)
    tokens = draw_tokens(jax.random.fold_in(jax.random.fold_in(streams_of[9], part), 71), part)
    norm_gain = jnp.clip(1.0 + 0.18 * jax.random.normal(streams_of[1], (D,), jnp.float32), 0.1, 1.9)
    query_weight = draw_query_weight(jax.random.fold_in(streams_of[9], 71), part)
    key_weight = draw_key_weight(jax.random.fold_in(streams_of[9], 71), part)
    value_weight = noise(streams_of[4], (D, KV_HEADS, HEAD_DIM), D ** -0.5, 0.125, ((1, 2),))
    sink_logit = jnp.clip(1.0 + 5.0 * jax.random.uniform(streams_of[5], (HEADS,), jnp.float32) ** block_levels(streams_of[5], (HEADS,), ((0, 2),), -0.2, 0.2), 1.0, 6.0)
    pool_weight = noise(streams_of[6], (D, 4, POOL_CH), D ** -0.5, 0.125, ((2, 2),))
    attn_out_weight = noise(streams_of[7], (HEADS, HEAD_DIM, D), (HEADS * HEAD_DIM // 8) ** -0.5, 0.5, ((0, 2),))
    pool_out_weight = noise(streams_of[8], (4, POOL_CH, D), (4 * POOL_CH) ** -0.5, 0.1875, ((1, 2),))
    return dict(tokens=tokens, norm_gain=norm_gain, query_weight=query_weight, key_weight=key_weight, value_weight=value_weight, sink_logit=sink_logit, pool_weight=pool_weight, attn_out_weight=attn_out_weight, pool_out_weight=pool_out_weight)


def rms_norm(rows, gain):
    values = rows.astype(jnp.float32)
    scale = lax.rsqrt(lax.optimization_barrier(jnp.mean(values * values, axis=-1, keepdims=True)) + 1e-06)
    return (values * scale * gain).astype(jnp.bfloat16)

def attend(query, key, value, sinks):
    group = HEADS // KV_HEADS
    blocks = LEN // WINDOW
    qb = query.reshape(blocks, WINDOW, KV_HEADS, group, HEAD_DIM).astype(jnp.float32)

    def banded(tensor):
        tb = tensor.reshape(blocks, WINDOW, KV_HEADS, HEAD_DIM)
        before = jnp.concatenate([jnp.zeros_like(tb[:1]), tb[:-1]], axis=0)
        return jnp.concatenate([before, tb], axis=1).astype(jnp.float32)
    kw = banded(key)
    vw = banded(value)
    qi = jnp.arange(WINDOW, dtype=jnp.int32)[:, None]
    kj = jnp.arange(2 * WINDOW, dtype=jnp.int32)[None, :]
    dist = WINDOW + qi - kj
    inside = (dist >= 0) & (dist < WINDOW)
    key_pos = jnp.arange(blocks, dtype=jnp.int32)[:, None, None] * WINDOW - WINDOW + kj[None]
    mask = inside[None] & (key_pos >= 0)
    scores = jnp.einsum('nqhgd,nkhd->nhgqk', qb, kw) * HEAD_DIM ** (-0.5)
    scores = jnp.where(mask[:, None, None], scores, -jnp.inf)
    sink = sinks.reshape(1, KV_HEADS, group, 1, 1)
    top = jnp.maximum(lax.optimization_barrier(jnp.max(scores, axis=-1, keepdims=True)), sink)
    expo = jnp.exp(scores - top)
    total = lax.optimization_barrier(jnp.sum(expo, axis=-1, keepdims=True)) + jnp.exp(sink - top)
    weight = (expo / total).astype(jnp.bfloat16)
    out = jnp.einsum('nhgqk,nkhd->nqhgd', weight.astype(jnp.float32), vw)
    return out.reshape(LEN, HEADS * HEAD_DIM).astype(jnp.bfloat16)

def pool(pooled_in):
    values = pooled_in.astype(jnp.float32)
    sums = jnp.cumsum(values, axis=0)
    count = jnp.arange(1, LEN + 1).astype(jnp.float32)[:, None]
    parts = []
    for group, reach in enumerate((2, 4, 16)):
        col = sums[:, group]
        lower = jnp.concatenate([jnp.zeros((reach, POOL_CH), jnp.float32), col[:-reach]], axis=0)
        parts.append((col - lower) / jnp.minimum(count, float(reach)))
    parts.append(sums[:, 3] / count)
    mean = jnp.stack(parts, axis=1)
    return (mean - values).astype(jnp.bfloat16)

def one_sequence(rows, norm_gain, query_weight, key_weight, value_weight, sink_logit, pool_weight, attn_out_weight, pool_out_weight):
    normed = rms_norm(rows, norm_gain)
    query = jnp.dot(normed, query_weight.reshape(D, -1), preferred_element_type=jnp.float32).astype(jnp.bfloat16)
    key = jnp.dot(normed, key_weight.reshape(D, -1), preferred_element_type=jnp.float32).astype(jnp.bfloat16)
    value = jnp.dot(normed, value_weight.reshape(D, -1), preferred_element_type=jnp.float32).astype(jnp.bfloat16)
    pooled_in = jnp.dot(normed, pool_weight.reshape(D, -1), preferred_element_type=jnp.float32).astype(jnp.bfloat16)
    attended = attend(query, key, value, sink_logit)
    pooled = pool(pooled_in.reshape(LEN, 4, POOL_CH)).reshape(LEN, 4 * POOL_CH)
    total = jnp.dot(attended, attn_out_weight.reshape(-1, D), preferred_element_type=jnp.float32)
    total = total + jnp.dot(pooled, pool_out_weight.reshape(-1, D), preferred_element_type=jnp.float32)
    return total.astype(jnp.bfloat16)

def reference(tokens, norm_gain, query_weight, key_weight, value_weight, sink_logit, pool_weight, attn_out_weight, pool_out_weight):

    def apply(rows):
        return one_sequence(rows, norm_gain, query_weight, key_weight, value_weight, sink_logit, pool_weight, attn_out_weight, pool_out_weight)
    return lax.map(apply, tokens)
```

```python
import jax
import jax.numpy as jnp
from jax import lax
from jax.sharding import PartitionSpec as P

WINDOW = 128


def from_behind(value, axis, steps):
    count = lax.axis_size(axis)
    return lax.ppermute(value, axis, [(i, (i + steps) % count) for i in range(count)])


def swap(value):
    return lax.ppermute(value, "tp", [(0, 1), (1, 0)])


def rms_norm(rows, gain):
    values = rows.astype(jnp.float32)
    scale = lax.rsqrt(jnp.mean(values * values, axis=-1, keepdims=True) + 1e-06)
    return (values * scale * gain).astype(jnp.bfloat16)


def attend(query, key, value, key_tail, value_tail, sinks, offset):
    rows = query.shape[0]
    local_kv = key_tail.shape[1]
    head_dim = key_tail.shape[2]
    group = query.shape[1] // (local_kv * head_dim)
    blocks = rows // WINDOW
    qb = query.reshape(blocks, WINDOW, local_kv, group, head_dim)

    def banded(tensor, tail):
        tb = tensor.reshape(blocks, WINDOW, local_kv, head_dim)
        whole = jnp.concatenate([tail, tensor.reshape(rows, local_kv, head_dim)], axis=0)
        before = whole[:rows].reshape(blocks, WINDOW, local_kv, head_dim)
        return jnp.concatenate([before, tb], axis=1)

    kw = banded(key, key_tail)
    vw = banded(value, value_tail)
    qi = jnp.arange(WINDOW, dtype=jnp.int32)[:, None]
    kj = jnp.arange(2 * WINDOW, dtype=jnp.int32)[None, :]
    dist = WINDOW + qi - kj
    inside = (dist >= 0) & (dist < WINDOW)
    key_pos = (
        offset + jnp.arange(blocks, dtype=jnp.int32)[:, None, None] * WINDOW - WINDOW + kj[None]
    )
    mask = inside[None] & (key_pos >= 0)
    scores = jnp.einsum(
        "nqhgd,nkhd->nhgqk", qb, kw, preferred_element_type=jnp.float32
    ) * head_dim ** (-0.5)
    scores = jnp.where(mask[:, None, None], scores, -jnp.inf)
    sink = sinks.reshape(1, local_kv, group, 1, 1)
    top = jnp.maximum(jnp.max(scores, axis=-1, keepdims=True), sink)
    expo = jnp.exp(scores - top)
    total = jnp.sum(expo, axis=-1, keepdims=True) + jnp.exp(sink - top)
    weight = (expo / total).astype(jnp.bfloat16)
    out = jnp.einsum("nhgqk,nkhd->nqhgd", weight, vw, preferred_element_type=jnp.float32)
    return out.reshape(rows, -1).astype(jnp.bfloat16)


def shards(
    tokens,
    norm_gain,
    query_weight,
    key_weight,
    value_weight,
    sink_logit,
    pool_weight,
    attn_out_weight,
    pool_out_weight,
):
    mine = tokens[0]
    other = swap(mine)
    side = lax.axis_index("tp")
    whole = jnp.concatenate(
        [jnp.where(side == 0, mine, other), jnp.where(side == 0, other, mine)], axis=1
    )
    rows = whole.shape[0]
    width = whole.shape[1]
    local_kv = key_weight.shape[1]
    head_dim = key_weight.shape[2]
    channels = pool_weight.shape[2]
    normed = rms_norm(whole, norm_gain)
    query = jnp.dot(
        normed, query_weight.reshape(width, -1), preferred_element_type=jnp.float32
    ).astype(jnp.bfloat16)
    key = jnp.dot(normed, key_weight.reshape(width, -1), preferred_element_type=jnp.float32).astype(
        jnp.bfloat16
    )
    value = jnp.dot(
        normed, value_weight.reshape(width, -1), preferred_element_type=jnp.float32
    ).astype(jnp.bfloat16)
    pooled_in = jnp.dot(
        normed, pool_weight.reshape(width, -1), preferred_element_type=jnp.float32
    ).astype(jnp.bfloat16)
    pool_rows = pooled_in.reshape(rows, 4, channels)
    key_rows = key.reshape(rows, local_kv, head_dim)
    value_rows = value.reshape(rows, local_kv, head_dim)
    place = lax.axis_index("sp")
    tails = jnp.concatenate(
        [key[rows - WINDOW :], value[rows - WINDOW :], pooled_in[rows - WINDOW :]], axis=1
    )
    tails = jnp.where(place > 0, from_behind(tails, "sp", 1), 0)
    narrow = local_kv * head_dim
    key_tail = tails[:, :narrow].reshape(WINDOW, local_kv, head_dim)
    value_tail = tails[:, narrow : 2 * narrow].reshape(WINDOW, local_kv, head_dim)
    pool_tail = tails[:, 2 * narrow :].reshape(WINDOW, 4, channels)
    offset = lax.axis_index("sp") * rows
    attended = attend(query, key, value, key_tail, value_tail, sink_logit, offset)
    prefix_total = jnp.sum(pool_rows[:, 3].astype(jnp.float32), axis=0)
    running = prefix_total
    carried = jnp.zeros_like(prefix_total)
    step = 1
    while step < lax.axis_size("sp"):
        got = jnp.where(place >= step, from_behind(running, "sp", step), 0.0)
        carried = carried + got
        running = running + got
        step *= 2
    reaches = jnp.array([2.0, 4.0, 16.0, 1000000000.0], jnp.float32)
    ext = jnp.concatenate([pool_tail, pool_rows], axis=0)
    position = jnp.arange(rows, dtype=jnp.int32)[:, None]
    source = jnp.arange(rows + WINDOW, dtype=jnp.int32)[None, :]
    gap = (position + WINDOW - source).astype(jnp.float32)
    group_ids = jnp.arange(4, dtype=jnp.int32)[:, None, None]
    band = (
        (gap[None] >= 0.0)
        & (gap[None] < reaches[:, None, None])
        & ((group_ids < 3) | (source[None] >= WINDOW))
    )
    sums = jnp.einsum(
        "gij,jgc->igc", band.astype(jnp.bfloat16), ext, preferred_element_type=jnp.float32
    )
    carry_rows = jnp.concatenate([jnp.zeros((3, channels), jnp.float32), carried[None]], axis=0)
    sums = sums + carry_rows[None]
    count = (offset + jnp.arange(1, rows + 1, dtype=jnp.int32)).astype(jnp.float32)
    denom = jnp.minimum(count[:, None], reaches[None, :])[:, :, None]
    pooled = (
        (sums / denom - pool_rows.astype(jnp.float32))
        .astype(jnp.bfloat16)
        .reshape(rows, 4 * channels)
    )
    attn_rows = attn_out_weight.reshape(-1, width)
    pool_weight_rows = pool_out_weight.reshape(-1, width)
    half = rows // 2

    def project(start):
        part = jnp.dot(
            lax.dynamic_slice_in_dim(attended, start, half, 0),
            attn_rows,
            preferred_element_type=jnp.float32,
        )
        return part + jnp.dot(
            lax.dynamic_slice_in_dim(pooled, start, half, 0),
            pool_weight_rows,
            preferred_element_type=jnp.float32,
        )

    given = swap(project((1 - side) * half).astype(jnp.bfloat16))
    result = (project(side * half) + given.astype(jnp.float32)).astype(jnp.bfloat16)
    return result[None]


def solution(mesh):
    in_specs = (
        P("fs", ("grp", "sp"), "tp"),
        P(),
        P(None, "tp", None),
        P(None, "tp", None),
        P(None, "tp", None),
        P("tp"),
        P(None, None, "tp"),
        P("tp", None, None),
        P(None, "tp", None),
    )
    out_specs = P("fs", ("grp", "sp", "tp"), None)
    return jax.shard_map(shards, mesh=mesh, in_specs=in_specs, out_specs=out_specs, check_vma=False)
```

```python
import functools

import jax
import jax.numpy as jnp
from jax import lax
from jax.experimental import pallas as pl
from jax.experimental.pallas import tpu as pltpu
from jax.sharding import PartitionSpec as P

WINDOW = 128
REACHES = (2, 4, 16)
BF16 = jnp.bfloat16
F32 = jnp.float32
VMEM = pl.BlockSpec(memory_space=pltpu.VMEM)
SMEM = pl.BlockSpec(memory_space=pltpu.SMEM)
ANY = pl.BlockSpec(memory_space=pl.ANY)


def from_behind(value, axis, steps):
    count = lax.axis_size(axis)
    return lax.ppermute(value, axis, [(i, (i + steps) % count) for i in range(count)])


def swap(value):
    return lax.ppermute(value, "tp", [(0, 1), (1, 0)])


def params(mib):
    return pltpu.CompilerParams(vmem_limit_bytes=mib * 2**20)


def dot(left, right, dims):
    return lax.dot_general(left, right, (dims, ((), ())), preferred_element_type=F32)


NN, NT, TN = ((1,), (0,)), ((1,), (1,)), ((0,), (0,))


def project_kernel(
    side_ref, gain_ref, mine, other, wq, wk, wv, wp,
    qkv_ref, pool_ref, tail_ref, total_ref,
    tokens, wqkv, wpool, normed, token_sem, weight_sem,
):
    rows, half = mine.shape
    queries, narrow, channels = wq.shape[0], wk.shape[0], wp.shape[1] // 4
    chunk = rows // 3 if rows % 3 == 0 else rows
    chunks = rows // chunk
    side = side_ref[0]
    token_copies = []
    for c in range(chunks):
        span = pl.ds(c * chunk, chunk)
        for i, source in enumerate((mine, other)):
            copy = pltpu.make_async_copy(
                source.at[span], tokens.at[i, span], token_sem.at[2 * c + i]
            )
            copy.start()
            token_copies.append(copy)
    weight_copies = [
        pltpu.make_async_copy(wq, wqkv.at[pl.ds(0, queries)], weight_sem.at[0]),
        pltpu.make_async_copy(wk, wqkv.at[pl.ds(queries, narrow)], weight_sem.at[1]),
        pltpu.make_async_copy(wv, wqkv.at[pl.ds(queries + narrow, narrow)], weight_sem.at[2]),
        pltpu.make_async_copy(wp, wpool, weight_sem.at[3]),
    ]
    for copy in weight_copies:
        copy.start()
    places = [pl.multiple_of(s * half, half) for s in (side, 1 - side)]
    gains = [gain_ref[:, pl.ds(place, half)] for place in places]
    block = 32

    def normalise(c):
        def body(i, _):
            span = pl.ds(pl.multiple_of(c * chunk + i * block, block), block)
            parts = [tokens[k, span, :].astype(F32) for k in range(2)]
            squares = sum(jnp.sum(part * part, axis=-1, keepdims=True) for part in parts)
            scale = lax.rsqrt(squares / (2 * half) + 1e-06)
            for part, gain, place in zip(parts, gains, places):
                normed[span, pl.ds(place, half)] = (part * scale * gain).astype(BF16)
            return 0

        lax.fori_loop(0, chunk // block, body, 0)

    for c in range(chunks):
        token_copies[2 * c].wait()
        token_copies[2 * c + 1].wait()
        normalise(c)
        if c == 0:
            for copy in weight_copies[:3]:
                copy.wait()
        span = pl.ds(c * chunk, chunk)
        qkv_ref[:, span] = dot(wqkv[...], normed[span, :], NT).astype(BF16)
    weight_copies[3].wait()
    step = 256
    for n in range(0, 4 * channels, step):
        pool_ref[:, n : n + step] = dot(normed[...], wpool[:, n : n + step], NN).astype(BF16)
    last = rows - WINDOW
    tail_ref[0 : 2 * narrow, :] = qkv_ref[queries:, last:]
    for g in range(3):
        at = 2 * narrow + 16 * g
        tail_ref[at : at + 16, :] = pool_ref[rows - 16 :, g * channels : (g + 1) * channels]
    total = jnp.sum(pool_ref[:, 3 * channels :].astype(F32), axis=0, keepdims=True)
    total_ref[...] = jnp.broadcast_to(total, total_ref.shape)


def project(side, gain, mine, other, wq, wk, wv, wp):
    rows, half = mine.shape
    width = 2 * half
    wide = wq.shape[0] + wk.shape[0] + wv.shape[0]
    channels = wp.shape[1] // 4
    chunks = 3 if rows % 3 == 0 else 1
    return pl.pallas_call(
        project_kernel,
        out_shape=(
            jax.ShapeDtypeStruct((wide, rows), BF16),
            jax.ShapeDtypeStruct((rows, 4 * channels), BF16),
            jax.ShapeDtypeStruct((2 * wk.shape[0] + 48, WINDOW), BF16),
            jax.ShapeDtypeStruct((8, channels), F32),
        ),
        in_specs=[SMEM, VMEM, ANY, ANY, ANY, ANY, ANY, ANY],
        out_specs=(VMEM,) * 4,
        scratch_shapes=[
            pltpu.VMEM((2, rows, half), BF16),
            pltpu.VMEM((wide, width), BF16),
            pltpu.VMEM((width, 4 * channels), BF16),
            pltpu.VMEM((rows, width), BF16),
            pltpu.SemaphoreType.DMA((2 * chunks,)),
            pltpu.SemaphoreType.DMA((4,)),
        ],
        compiler_params=params(32),
        cost_estimate=pl.CostEstimate(
            flops=2 * rows * width * (wide + 4 * channels),
            bytes_accessed=2 * (rows + wide + 4 * channels) * width,
            transcendentals=rows,
        ),
        name="project",
    )(side, gain, mine, other, wq, wk, wv, wp)


def attend_block(queries, keys, values, sinks_ref, valid):
    head_dim = 64
    heads = queries.shape[0] // head_dim
    local_kv = keys[0].shape[0] // head_dim
    group = heads // local_kv
    zero = jnp.zeros((head_dim, WINDOW), BF16)
    wide = jnp.concatenate(
        [
            jnp.concatenate(
                [
                    queries[h * head_dim : (h + 1) * head_dim] if h // group == v else zero
                    for h in range(heads)
                ],
                axis=1,
            )
            for v in range(local_kv)
        ],
        axis=0,
    )
    before = dot(keys[0], wide, TN)
    here = dot(keys[1], wide, TN)
    older = lax.broadcasted_iota(jnp.int32, (WINDOW, WINDOW), 0) > lax.broadcasted_iota(
        jnp.int32, (WINDOW, WINDOW), 1
    )
    outs = []
    for v in range(local_kv):
        olds, news = [], []
        for h in range(v * group, (v + 1) * group):
            lanes = slice(h * WINDOW, (h + 1) * WINDOW)
            past = before[:, lanes]
            if valid is not None:
                past = jnp.where(valid, past, -jnp.inf)
            score = jnp.where(older, past, here[:, lanes]) * head_dim ** (-0.5)
            sink = sinks_ref[h]
            top = jnp.maximum(jnp.max(score, axis=0, keepdims=True), sink)
            expo = jnp.exp(score - top)
            total = jnp.sum(expo, axis=0, keepdims=True) + jnp.exp(sink - top)
            weight = expo * (1.0 / total)
            olds.append(jnp.where(older, weight, 0.0).astype(BF16))
            news.append(jnp.where(older, 0.0, weight).astype(BF16))
        mine = slice(v * head_dim, (v + 1) * head_dim)
        out = dot(values[0][mine], jnp.concatenate(olds, axis=1), NN) + dot(
            values[1][mine], jnp.concatenate(news, axis=1), NN
        )
        outs += [out[:, g * WINDOW : (g + 1) * WINDOW] for g in range(group)]
    return jnp.concatenate(outs, axis=0).astype(BF16)


def attend_kernel(sinks_ref, qkv_ref, out_ref):
    wide, rows = qkv_ref.shape
    queries = out_ref.shape[0]
    narrow = (wide - queries) // 2

    def body(b, _):
        here = pl.ds(pl.multiple_of(b * WINDOW, WINDOW), WINDOW)
        past = pl.ds(pl.multiple_of((b - 1) * WINDOW, WINDOW), WINDOW)
        keys = [qkv_ref[queries : queries + narrow, s] for s in (past, here)]
        values = [qkv_ref[queries + narrow :, s] for s in (past, here)]
        out_ref[:, past] = attend_block(qkv_ref[:queries, here], keys, values, sinks_ref, None)
        return 0

    lax.fori_loop(1, rows // WINDOW, body, 0)


def attend(sinks, qkv, queries):
    wide, rows = qkv.shape
    return pl.pallas_call(
        attend_kernel,
        out_shape=jax.ShapeDtypeStruct((queries, rows - WINDOW), BF16),
        in_specs=[SMEM, VMEM],
        out_specs=VMEM,
        compiler_params=params(16),
        cost_estimate=pl.CostEstimate(
            flops=3 * 10**9, bytes_accessed=2 * wide * rows, transcendentals=rows * 1024
        ),
        name="attend",
    )(sinks, qkv)


def finish_kernel(sinks_ref, place_ref, qkv_ref, pool_ref, tail_ref, carry_ref, out_ref, pooled_ref, ext):
    wide, rows = qkv_ref.shape
    queries = out_ref.shape[0]
    narrow = (wide - queries) // 2
    channels = pool_ref.shape[1] // 4
    place = place_ref[0]
    here = slice(0, WINDOW)
    keys = [tail_ref[:narrow, :], qkv_ref[queries : queries + narrow, here]]
    values = [tail_ref[narrow : 2 * narrow, :], qkv_ref[queries + narrow :, here]]
    out_ref[...] = attend_block(qkv_ref[:queries, here], keys, values, sinks_ref, place > 0)

    count = (
        lax.broadcasted_iota(jnp.int32, (rows, channels), 0) + (place * rows + 1)
    ).astype(F32)
    for g, reach in enumerate(REACHES):
        lanes = slice(g * channels, (g + 1) * channels)
        at = 2 * narrow + 16 * g
        ext[0:16, :] = jnp.zeros((16, channels), F32)
        ext[16:32, :] = jnp.where(place > 0, tail_ref[at : at + 16, :].astype(F32), 0.0)
        ext[32:, :] = pool_ref[:, lanes].astype(F32)
        low = 1
        while low < reach:
            ext[8:, :] = ext[8:, :] + ext[8 - low : 32 + rows - low, :]
            low *= 2
        summed = ext[32:, :]
        own = pool_ref[:, lanes].astype(F32)
        mean = summed / jnp.minimum(count, float(reach))
        pooled_ref[:, lanes] = (mean - own).astype(BF16)
    lanes = slice(3 * channels, 4 * channels)
    blocks = rows // WINDOW
    lower = (
        lax.broadcasted_iota(jnp.int32, (WINDOW, WINDOW), 0)
        >= lax.broadcasted_iota(jnp.int32, (WINDOW, WINDOW), 1)
    ).astype(BF16)
    side_by_side = jnp.concatenate(
        [pool_ref[b * WINDOW : (b + 1) * WINDOW, lanes] for b in range(blocks)], axis=1
    )
    sums = dot(lower, side_by_side, NN)
    running = carry_ref[0:1, :]
    for b in range(blocks):
        span = slice(b * WINDOW, (b + 1) * WINDOW)
        inner = sums[:, b * channels : (b + 1) * channels]
        mean = (inner + running) / count[span]
        pooled_ref[span, lanes] = (mean - pool_ref[span, lanes].astype(F32)).astype(BF16)
        running = running + inner[WINDOW - 1 :, :]


def finish(sinks, place, qkv, pool, tail, carry, queries):
    wide, rows = qkv.shape
    channels = pool.shape[1] // 4
    return pl.pallas_call(
        finish_kernel,
        out_shape=(
            jax.ShapeDtypeStruct((queries, WINDOW), BF16),
            jax.ShapeDtypeStruct(pool.shape, BF16),
        ),
        in_specs=[SMEM, SMEM, VMEM, VMEM, VMEM, VMEM],
        out_specs=(VMEM, VMEM),
        scratch_shapes=[pltpu.VMEM((rows + 32, channels), F32)],
        compiler_params=params(24),
        cost_estimate=pl.CostEstimate(
            flops=10**9, bytes_accessed=2 * wide * rows, transcendentals=1024 * 128
        ),
        name="finish",
    )(sinks, place, qkv, pool, tail, carry)


def shards(
    tokens,
    norm_gain,
    query_weight,
    key_weight,
    value_weight,
    sink_logit,
    pool_weight,
    attn_out_weight,
    pool_out_weight,
):
    mine = tokens[0]
    other = swap(mine)
    rows = mine.shape[0]
    width = norm_gain.shape[0]
    side = lax.axis_index("tp")
    place = lax.axis_index("sp")

    def rows_of(weight):
        return weight.transpose(1, 2, 0).reshape(-1, width)

    qkv, pool, tail, total = project(
        side[None],
        norm_gain[None],
        mine,
        other,
        rows_of(query_weight),
        rows_of(key_weight),
        rows_of(value_weight),
        pool_weight.reshape(width, -1),
    )
    queries = query_weight.shape[1] * query_weight.shape[2]
    tail = from_behind(tail, "sp", 1)
    count = lax.axis_size("sp")
    carried = jnp.zeros_like(total)
    if count <= 4:
        for steps in range(1, count):
            got = from_behind(total, "sp", steps)
            carried = carried + jnp.where(place >= steps, got, 0.0)
    else:
        running = total
        steps = 1
        while steps < count:
            got = jnp.where(place >= steps, from_behind(running, "sp", steps), 0.0)
            carried = carried + got
            running = running + got
            steps *= 2
    later = attend(sink_logit, qkv, queries)
    first, pooled = finish(sink_logit, place[None], qkv, pool, tail, carried, queries)
    attended = jnp.concatenate([first, later], axis=1)
    attn_rows = attn_out_weight.reshape(-1, width)
    pool_weight_rows = pool_out_weight.reshape(-1, width)
    half = rows // 2

    def merge(start):
        part = dot(lax.dynamic_slice_in_dim(attended, start, half, 1), attn_rows, TN)
        return part + dot(lax.dynamic_slice_in_dim(pooled, start, half, 0), pool_weight_rows, NN)

    given = swap(merge((1 - side) * half).astype(BF16))
    result = (merge(side * half) + given.astype(F32)).astype(BF16)
    return result[None]


def solution(mesh):
    in_specs = (
        P("fs", ("grp", "sp"), "tp"),
        P(),
        P(None, "tp", None),
        P(None, "tp", None),
        P(None, "tp", None),
        P("tp"),
        P(None, None, "tp"),
        P("tp", None, None),
        P(None, "tp", None),
    )
    out_specs = P("fs", ("grp", "sp", "tp"), None)
    return jax.shard_map(shards, mesh=mesh, in_specs=in_specs, out_specs=out_specs, check_vma=False)
```
